32 devices in a mesh: fs: 8 (over z, core), tp: 4 (over y, x).
Axes of the slice: x: 2, y: 2, z: 4, core: 2. Of those that a mesh axis runs over, the one named last changes fastest.
Arguments:
- tokens: bfloat16 [2048, 2048], P('fs'), may hold values from -6 to 6
- routes: int32 [2048, 2], P('fs'), may hold values from 0 to 3, all different within a row
- route_logits: float32 [2048, 2], P('fs'), may hold values from -6 to 6
- norm_gain: float32 [2048], P('fs'), may hold values from 0.1 to 1.9
- gate_weight: float32 [2048, 8192], P('fs', 'tp')
- up_weight: float32 [2048, 8192], P('fs', 'tp')
- down_weight: float32 [2048, 8192], P('fs', 'tp'), may hold values from -0.125 to 0.125
Outputs:
- gate_sampler: bfloat16 [2048, 8192], P(None, 'tp')
- up_sampler: bfloat16 [2048, 8192], P(None, 'tp')
- down_sampler: bfloat16 [2048, 8192], P(None, 'tp')
- moe_out: bfloat16 [2048, 2048], P('fs', 'tp')
The draws below stay inside these ranges and needn't reach their ends.
Inputs may be any that keep to these rules, and one draw needn't show every extreme that they name: `routes`: each row names 2 different experts; every expert is named by some row.
All inputs are finite; a program needn't handle non-finite values.
Results may differ from the reference program's by a relative error of at most 0.014.
Values may be sent and summed in bfloat16 or wider, within the bound.
A program may use at most 128 MiB of HBM per device.

```python
import math
import jax
import jax.numpy as jnp
from jax import lax

D = 2048
FF = 2048
EXPERTS = 4
TOP = 2
TOKENS = 2048
HID = 2048
N_TP = 4


def column_scaled(key, salt):
    inner = jax.random.fold_in(key, salt)
    first_key, second_key = jax.random.split(inner)
    scales = jnp.exp(jax.random.uniform(second_key, (EXPERTS * FF,), jnp.float32, 0.0, math.log(8.0)))
    values = jax.random.normal(first_key, (D, EXPERTS * FF), jnp.float32)
    return values * D ** (-0.5) * scales[None, :]


def draw_gate_weight(key, part):
    return column_scaled(key, 11)


def draw_up_weight(key, part):
    return column_scaled(key, 23)


def shard_levels(rng, extent, pieces, least, high):
    gain = 1.0
    for dim, shards_of in pieces:
        draws = jax.random.uniform(jax.random.fold_in(jax.random.fold_in(rng, 6), dim), (shards_of,), jnp.float32, least / len(pieces), high / len(pieces))
        gain = gain * jnp.repeat(jnp.exp(draws), extent[dim] // shards_of).reshape((-1,) + (1,) * (len(extent) - 1 - dim))
    return gain


def different_ones(stream_key, rows, count, top, lift):
    ranking = jax.random.permutation(jax.random.fold_in(stream_key, 1), count)
    favour = ranking
    for power in range(3):
        favour = favour * favour // count
    favour = favour * lift // count
    lots = jax.random.randint(jax.random.fold_in(stream_key, 2), (rows, count), 0, 4096) + favour
    fixed_rows = jax.random.permutation(jax.random.fold_in(stream_key, 3), rows)[jnp.arange(count) % rows]
    lots = jnp.where(jnp.arange(rows)[:, None] == fixed_rows[None, :], 1 << 14, lots)
    score = lots * count + jnp.arange(count)
    return lax.top_k(score.astype(jnp.int32), top)[1].astype(jnp.int32)


def normal_values(rng, extent, deviation, reach, pieces=(), dtype=jnp.bfloat16):
    values = jax.random.normal(rng, extent, jnp.float32) * deviation
    if len(pieces) > 0:
        values = shard_levels(rng, extent, pieces, -0.22, 0.18) * values
    return jnp.clip(values, min=-reach, max=reach).astype(dtype)


def setup_inputs(seed: int = 0) -> dict:
    keys = jax.random.split(jax.random.key(seed), 8)
    return {
        "tokens": normal_values(keys[0], (TOKENS, D), 1.0, 6.0, ((0, 8),)),
        "routes": different_ones(keys[1], TOKENS, EXPERTS, TOP, 0),
        "route_logits": normal_values(keys[2], (TOKENS, TOP), 1.5, 6.0, ((0, 8),), jnp.float32),
        "norm_gain": jnp.clip(1.0 + 0.18 * jax.random.normal(keys[3], (D,), jnp.float32), 0.1, 1.9),
        "gate_weight": draw_gate_weight(jax.random.fold_in(keys[7], 71), 0),
        "up_weight": draw_up_weight(jax.random.fold_in(keys[7], 71), 0),
        "down_weight": normal_values(keys[6], (D, EXPERTS * FF), FF ** -0.5, 0.125, ((0, 8), (1, 4)), jnp.float32),
    }


EPSILON = 1e-06
CLAMP_LIMIT = 7.0
SIGMOID_SCALE = 1.702

def clamped_unit(pre_gate, pre_up):
    gated = jnp.minimum(pre_gate, CLAMP_LIMIT)
    upper = jnp.clip(pre_up, -CLAMP_LIMIT, CLAMP_LIMIT)
    return gated * jax.nn.sigmoid(SIGMOID_SCALE * gated) * (upper + 1.0)

def reference(tokens, routes, route_logits, norm_gain, gate_weight, up_weight, down_weight):
    gate_cast = (norm_gain[:, None] * gate_weight).astype(jnp.bfloat16)
    up_cast = (norm_gain[:, None] * up_weight).astype(jnp.bfloat16)
    down_cast = down_weight.astype(jnp.bfloat16)
    widened = tokens.astype(jnp.float32)
    normed = (widened * lax.rsqrt(lax.optimization_barrier(jnp.mean(widened * widened, axis=-1, keepdims=True)) + EPSILON)).astype(jnp.bfloat16)
    shares = jax.nn.softmax(route_logits.astype(jnp.float32), axis=-1)

    def add_group(group, summed):
        first = (group * HID).astype(jnp.int32)
        expert = (first // FF).astype(jnp.int32)
        weight = lax.optimization_barrier(jnp.sum(jnp.where(routes == expert, shares, jnp.float32(0.0)), axis=-1, keepdims=True))
        gate_part = lax.dynamic_slice_in_dim(gate_cast, first, HID, 1)
        up_part = lax.dynamic_slice_in_dim(up_cast, first, HID, 1)
        down_part = lax.dynamic_slice_in_dim(down_cast, first, HID, 1)
        pre_gate = jnp.dot(normed, gate_part, preferred_element_type=jnp.float32)
        pre_up = jnp.dot(normed, up_part, preferred_element_type=jnp.float32)
        active = (weight * clamped_unit(pre_gate, pre_up)).astype(jnp.bfloat16)
        partial_value = jnp.dot(active, jnp.transpose(down_part), preferred_element_type=jnp.float32).astype(jnp.bfloat16)
        return summed + partial_value.astype(jnp.float32)
    summed = lax.fori_loop(jnp.int32(0), jnp.int32(N_TP), add_group, jnp.zeros((tokens.shape[0], tokens.shape[1]), jnp.float32))
    return (gate_cast, up_cast, down_cast, summed.astype(jnp.bfloat16))
```

```python
import functools

import jax
import jax.numpy as jnp
from jax import lax
from jax.experimental import pallas as pl
from jax.experimental.pallas import tpu as pltpu
from jax.sharding import PartitionSpec as P

FF = 2048
CORES = 2

EPSILON = 1e-06
CLAMP_LIMIT = 7.0
SIGMOID_SCALE = 1.702
MESH = pl.DeviceIdType.MESH
LEFT, RIGHT, PARTNER = range(3)


def clamped_unit(pre_gate, pre_up):
    gated = jnp.minimum(pre_gate, CLAMP_LIMIT)
    upper = jnp.clip(pre_up, -CLAMP_LIMIT, CLAMP_LIMIT)
    return gated * jax.nn.sigmoid(SIGMOID_SCALE * gated) * (upper + 1.0)


def kernel(
    n_fs, n_tp, chunk,
    tokens, routes, logits, gain, gate_w, up_w, down_w,
    gate_out, up_out, down_out, moe_out,
    staged, gain_col, normed, acc, active, part, landed,
    load_sem, send_sem, recv_sem, part_send, part_recv,
):
    me, tp = lax.axis_index("fs"), lax.axis_index("tp")
    z, core = me // CORES, me % CORES
    n_z = n_fs // CORES
    partner = z * CORES + (1 - core)
    weights, outs = (gate_w, up_w, down_w), (gate_out, up_out, down_out)
    rows, cols = gate_w.shape
    n_tokens, width = tokens.shape
    n_chunks = rows // chunk
    per_owner = width // n_tp

    barrier = pltpu.get_barrier_semaphore()

    def greet(device):
        pl.semaphore_signal(barrier, inc=1, device_id=device, device_id_type=MESH)

    pl.when(z > 0)(lambda: greet({"fs": me - CORES}))
    pl.when(z < n_z - 1)(lambda: greet({"fs": me + CORES}))
    greet({"fs": partner})
    for step in range(1, n_tp):
        greet({"tp": lax.rem(tp + step, n_tp)})

    def load(a, r):
        return pltpu.make_async_copy(
            weights[a].at[pl.ds(r * chunk, chunk)],
            staged.at[a, pl.ds(r * chunk, chunk)],
            load_sem.at[a, r],
        )

    for a in range(3):
        for r in range(n_chunks):
            load(a, r).start()

    here = lax.broadcasted_iota(jnp.int32, (rows, rows), 0)
    there = lax.broadcasted_iota(jnp.int32, (rows, rows), 1)
    gain_col[...] = jnp.sum(
        jnp.where(here == there, jnp.broadcast_to(gain[...], (rows, rows)), 0.0),
        axis=1, keepdims=True,
    )

    def place(s, r):
        return pl.ds(pl.multiple_of(s * rows + r * chunk, chunk), chunk)

    def copy(kind, a, s, r):
        target = (me - CORES, me + CORES, partner)[kind]
        return pltpu.make_async_remote_copy(
            src_ref=outs[a].at[place(s, r)],
            dst_ref=outs[a].at[place(s, r)],
            send_sem=send_sem.at[kind, a, s // CORES, r],
            recv_sem=recv_sem.at[a, s, r],
            device_id={"fs": target},
            device_id_type=MESH,
        )

    def send_own(a, r):
        pl.when(z > 0)(lambda: copy(LEFT, a, me, r).start())
        pl.when(z < n_z - 1)(lambda: copy(RIGHT, a, me, r).start())
        copy(PARTNER, a, me, r).start()

    own = [(a, r) for a in range(3) for r in range(n_chunks)]
    for i, (a, r) in enumerate(own):
        load(a, r).wait()
        block = staged[a, r * chunk : (r + 1) * chunk, :]
        if a < 2:
            block = gain_col[r * chunk : (r + 1) * chunk, :] * block
        outs[a][place(me, r), :] = block.astype(jnp.bfloat16)
        if i == 0:
            pl.semaphore_wait(
                barrier,
                n_tp + (z > 0).astype(jnp.int32) + (z < n_z - 1).astype(jnp.int32),
            )
        else:
            send_own(*own[i - 1])

    tile = min(32, n_tokens)

    def norm_tile(i, carry):
        at = pl.ds(pl.multiple_of(i * tile, tile), tile)
        wide = tokens[at, :].astype(jnp.float32)
        scale = lax.rsqrt(jnp.mean(wide * wide, axis=-1, keepdims=True) + EPSILON)
        value = (wide * scale).astype(jnp.bfloat16)
        for s in range(n_fs):
            normed[s, at, :] = value[:, s * rows : (s + 1) * rows]
        acc[0, at, :] = jnp.zeros((tile, cols), jnp.float32)
        acc[1, at, :] = jnp.zeros((tile, cols), jnp.float32)
        return carry

    lax.fori_loop(0, 1, norm_tile, 0)
    send_own(*own[-1])
    lax.fori_loop(1, n_tokens // tile, norm_tile, 0)

    wide_tile = min(512, cols)

    def project(a, s):
        block = pl.ds(pl.multiple_of(s * rows, rows), rows)

        def one(i, carry):
            at = pl.ds(pl.multiple_of(i * wide_tile, wide_tile), wide_tile)
            acc[a, :, at] += jnp.dot(
                normed[s], outs[a][block, at], preferred_element_type=jnp.float32
            )
            return carry

        lax.fori_loop(0, cols // wide_tile, one, 0)

    def wait_partner_line(a, s, r):
        copy(PARTNER, a, s, r).wait_recv()

    def wait_partner_block(a, s):
        def one(r, carry):
            wait_partner_line(a, s, r)
            return carry

        lax.fori_loop(0, n_chunks, one, 0)

    def project_pair(a, at_z):
        project(a, at_z * CORES + core)
        other = at_z * CORES + 1 - core
        wait_partner_block(a, other)
        project(a, other)

    def part_copy(s, r):
        start = s * rows + r * chunk
        owner, offset = start // per_owner, start % per_owner
        return pltpu.make_async_remote_copy(
            src_ref=part.at[pl.ds(pl.multiple_of(start, chunk), chunk)],
            dst_ref=landed.at[tp, pl.ds(pl.multiple_of(offset, chunk), chunk)],
            send_sem=part_send.at[s, r],
            recv_sem=part_recv.at[tp, offset // chunk],
            device_id={"tp": owner},
            device_id_type=MESH,
        )

    def down_rows(s, first, count):
        start = s * rows + first * chunk
        size = count * chunk
        at = pl.ds(pl.multiple_of(start, size), size)
        value = lax.dot_general(
            outs[2][at, :], active[...], (((1,), (1,)), ((), ())),
            preferred_element_type=jnp.float32,
        ).astype(jnp.bfloat16)
        owner, offset = start // per_owner, start % per_owner

        @pl.when(owner == tp)
        def _():
            landed[tp, pl.ds(pl.multiple_of(offset, size), size), :] = value

        @pl.when(owner != tp)
        def _():
            part[at, :] = value
            for r in range(count):
                part_copy(s, first + r).start()

    def activate():
        expert = tp * cols // FF

        def one(i, carry):
            at = pl.ds(pl.multiple_of(i * tile, tile), tile)
            score = logits[at, :]
            grown = jnp.exp(score - jnp.max(score, axis=-1, keepdims=True))
            shares = grown / jnp.sum(grown, axis=-1, keepdims=True)
            weight = jnp.sum(
                jnp.where(routes[at, :] == expert, shares, 0.0), axis=-1, keepdims=True
            )
            active[at, :] = (weight * clamped_unit(acc[0, at, :], acc[1, at, :])).astype(
                jnp.bfloat16
            )
            return carry

        lax.fori_loop(0, n_tokens // tile, one, 0)

    def down_near(s, carry):
        at_z = s // CORES

        @pl.when(jnp.abs(at_z - z) < n_z - 1)
        def _():
            pl.when(s % CORES != core)(lambda: wait_partner_block(2, s))
            down_rows(s, 0, n_chunks)

        return carry

    for a in range(2):
        project_pair(a, z)

    for d in range(1, n_z):
        last = d == n_z - 1
        for a in range(3):
            if last and a == 2:
                activate()
                lax.fori_loop(0, n_fs, down_near, 0)

            def arrive(r, carry, a=a, d=d, last=last):
                for sign, inside, onward, more in (
                    (-1, z - d >= 0, RIGHT, z < n_z - 1),
                    (1, z + d < n_z, LEFT, z > 0),
                ):

                    @pl.when(inside)
                    def _():
                        at_z = z + sign * d
                        s = at_z * CORES + core
                        copy(onward, a, s, r).wait_recv()
                        pl.when(more)(lambda: copy(onward, a, s, r).start())
                        copy(PARTNER, a, s, r).start()
                        if last and a == 2:
                            other = at_z * CORES + 1 - core
                            down_rows(s, r, 1)
                            wait_partner_line(a, other, r)
                            down_rows(other, r, 1)

                return carry

            lax.fori_loop(0, n_chunks, arrive, 0)
            if a < 2:
                pl.when(z - d >= 0)(lambda a=a, d=d: project_pair(a, z - d))
                pl.when(z + d < n_z)(lambda a=a, d=d: project_pair(a, z + d))

    for step in range(1, n_tp):
        sender = lax.rem(tp + step, n_tp)
        for j in range(per_owner // chunk):
            spot = landed.at[sender, pl.ds(j * chunk, chunk)]
            pltpu.make_async_remote_copy(
                src_ref=spot, dst_ref=spot, send_sem=part_send.at[0, 0],
                recv_sem=part_recv.at[sender, j],
                device_id={"tp": sender}, device_id_type=MESH,
            ).wait_recv()
    total = landed[0].astype(jnp.float32)
    for p in range(1, n_tp):
        total += landed[p].astype(jnp.float32)
    moe_out[...] = jnp.transpose(total).astype(jnp.bfloat16)

    def sent(s, carry):
        at_z = s // CORES

        def one(r, carry):
            @pl.when(s % CORES == core)
            def _():
                for a in range(3):
                    copy(PARTNER, a, s, r).wait_send()
                    pl.when((z > 0) & (at_z >= z))(lambda: copy(LEFT, a, s, r).wait_send())
                    pl.when((z < n_z - 1) & (at_z <= z))(
                        lambda: copy(RIGHT, a, s, r).wait_send()
                    )

            @pl.when((s * rows + r * chunk) // per_owner != tp)
            def _():
                part_copy(s, r).wait_send()

            return carry

        return lax.fori_loop(0, n_chunks, one, carry)

    lax.fori_loop(0, n_fs, sent, 0)


def write_out(*refs):
    count = (len(refs) - 1) // 2
    sources, targets, sem = refs[:count], refs[count:-1], refs[-1]
    copies = [
        pltpu.make_async_copy(source, target, sem.at[i])
        for i, (source, target) in enumerate(zip(sources, targets))
    ]
    for copy in copies:
        copy.start()
    for copy in copies:
        copy.wait()


def on_device(n_fs, n_tp, tokens, routes, logits, gain, gate_w, up_w, down_w):
    rows, cols = gate_w.shape
    n_tokens, width = tokens.shape
    per_owner = width // n_tp
    chunk = min(64, rows, per_owner)
    n_chunks = rows // chunk
    full = pltpu.VMEM((rows * n_fs, cols), jnp.bfloat16)
    vmem = pl.BlockSpec(memory_space=pltpu.VMEM)
    hbm = pl.BlockSpec(memory_space=pl.ANY)
    held = pl.pallas_call(
        functools.partial(kernel, n_fs, n_tp, chunk),
        out_shape=(full, full, full, pltpu.VMEM((n_tokens, per_owner), jnp.bfloat16)),
        in_specs=[vmem] * 4 + [hbm] * 3,
        out_specs=(vmem,) * 4,
        scratch_shapes=[
            pltpu.VMEM((3, rows, cols), jnp.float32),
            pltpu.VMEM((rows, 1), jnp.float32),
            pltpu.VMEM((n_fs, n_tokens, rows), jnp.bfloat16),
            pltpu.VMEM((2, n_tokens, cols), jnp.float32),
            pltpu.VMEM((n_tokens, cols), jnp.bfloat16),
            pltpu.VMEM((width, n_tokens), jnp.bfloat16),
            pltpu.VMEM((n_tp, per_owner, n_tokens), jnp.bfloat16),
            pltpu.SemaphoreType.DMA((3, n_chunks)),
            pltpu.SemaphoreType.DMA((3, 3, n_fs // CORES, n_chunks)),
            pltpu.SemaphoreType.DMA((3, n_fs, n_chunks)),
            pltpu.SemaphoreType.DMA((n_fs, n_chunks)),
            pltpu.SemaphoreType.DMA((n_tp, per_owner // chunk)),
        ],
        compiler_params=pltpu.CompilerParams(
            collective_id=0, has_side_effects=True, vmem_limit_bytes=34 * 2**20
        ),
    )(tokens, routes, logits, gain.reshape(1, rows), gate_w, up_w, down_w)
    return tuple(pl.pallas_call(
        write_out,
        out_shape=tuple(jax.ShapeDtypeStruct(x.shape, x.dtype) for x in held),
        in_specs=[hbm] * 4,
        out_specs=(hbm,) * 4,
        scratch_shapes=[pltpu.SemaphoreType.DMA((4,))],
        compiler_params=pltpu.CompilerParams(vmem_limit_bytes=2**20),
    )(*held))


def solution(mesh):
    return jax.shard_map(
        functools.partial(on_device, mesh.shape["fs"], mesh.shape["tp"]),
        mesh=mesh,
        in_specs=(
            P("fs", None),
            P("fs", None),
            P("fs", None),
            P("fs"),
            P("fs", "tp"),
            P("fs", "tp"),
            P("fs", "tp"),
        ),
        out_specs=(P(None, "tp"), P(None, "tp"), P(None, "tp"), P("fs", "tp")),
        check_vma=False,
    )
```

```python
import functools
import math

import jax
import jax.numpy as jnp
from jax import lax
from jax.experimental import pallas as pl
from jax.experimental.pallas import tpu as pltpu
from jax.sharding import PartitionSpec as P

FF = 2048
CORES = 2

EPSILON = 1e-06
CLAMP_LIMIT = 7.0
SIGMOID_SCALE = 1.702
MESH = pl.DeviceIdType.MESH
LEFT, RIGHT, PARTNER = range(3)


def clamped_unit(pre_gate, pre_up):
    gated = jnp.minimum(pre_gate, CLAMP_LIMIT)
    upper = jnp.clip(pre_up, -CLAMP_LIMIT, CLAMP_LIMIT)
    return gated * jax.nn.sigmoid(SIGMOID_SCALE * gated) * (upper + 1.0)


def as_column(row):
    n = row.shape[1]
    here = lax.broadcasted_iota(jnp.int32, (n, n), 0)
    there = lax.broadcasted_iota(jnp.int32, (n, n), 1)
    spread = jnp.where(here == there, jnp.broadcast_to(row, (n, n)), 0.0)
    return jnp.sum(spread, axis=1, keepdims=True)


def cuts(rows):
    if rows % 256:
        return [[(0, rows)]] * 3
    tables = []
    for parts in ((1, 2, 2, 3), (2, 2, 2, 2), (2, 2, 3, 1)):
        table, start = [], 0
        for part in parts:
            table.append((start, part * rows // 8))
            start += part * rows // 8
        tables.append(table)
    return tables


def kernel(
    n_fs, n_tp,
    tokens, routes, logits, gain, gate_w, up_w, down_w,
    gate_out, up_out, down_out, moe_out,
    staged, gain_col, weight_col, normed, acc, active, part, landed,
    load_sem, send_sem, recv_sem, part_send, part_recv,
):
    me, tp = lax.axis_index("fs"), lax.axis_index("tp")
    z, core = me // CORES, me % CORES
    n_z = n_fs // CORES
    partner = z * CORES + (1 - core)
    weights, outs = (gate_w, up_w, down_w), (gate_out, up_out, down_out)
    rows, cols = gate_w.shape
    n_tokens, width = tokens.shape
    table = cuts(rows)
    n_chunks = len(table[0])
    per_owner = width // n_tp

    barrier = pltpu.get_barrier_semaphore()

    def greet(device):
        pl.semaphore_signal(barrier, inc=1, device_id=device, device_id_type=MESH)

    pl.when(z > 0)(lambda: greet({"fs": me - CORES}))
    pl.when(z < n_z - 1)(lambda: greet({"fs": me + CORES}))
    greet({"fs": partner})
    for step in range(1, n_tp):
        greet({"tp": lax.rem(tp + step, n_tp)})

    def load(a, r):
        return pltpu.make_async_copy(
            weights[a].at[pl.ds(*table[a][r])],
            staged.at[a, pl.ds(*table[a][r])],
            load_sem.at[a, r],
        )

    for a in range(3):
        for r in range(n_chunks):
            load(a, r).start()

    gain_col[...] = as_column(gain[...])

    def place(a, s, r):
        first, size = table[a][r]
        return pl.ds(pl.multiple_of(s * rows + first, math.gcd(rows, first)), size)

    def copy(kind, a, s, r):
        target = (me - CORES, me + CORES, partner)[kind]
        return pltpu.make_async_remote_copy(
            src_ref=outs[a].at[place(a, s, r)],
            dst_ref=outs[a].at[place(a, s, r)],
            send_sem=send_sem.at[kind, a, s // CORES, r],
            recv_sem=recv_sem.at[a, s, r],
            device_id={"fs": target},
            device_id_type=MESH,
        )

    def send_own(a, r):
        pl.when(z > 0)(lambda: copy(LEFT, a, me, r).start())
        pl.when(z < n_z - 1)(lambda: copy(RIGHT, a, me, r).start())
        copy(PARTNER, a, me, r).start()

    own = [(a, r) for a in range(3) for r in range(n_chunks)]
    for i, (a, r) in enumerate(own):
        load(a, r).wait()
        at = pl.ds(*table[a][r])
        block = staged[a, at, :]
        if a < 2:
            block = gain_col[at, :] * block
        outs[a][place(a, me, r), :] = block.astype(jnp.bfloat16)
        if i == 0:
            pl.semaphore_wait(
                barrier,
                n_tp + (z > 0).astype(jnp.int32) + (z < n_z - 1).astype(jnp.int32),
            )
        else:
            send_own(*own[i - 1])

    tile = min(32, n_tokens)

    def norm_tile(i, carry):
        at = pl.ds(pl.multiple_of(i * tile, tile), tile)
        wide = tokens[at, :].astype(jnp.float32)
        scale = lax.rsqrt(jnp.mean(wide * wide, axis=-1, keepdims=True) + EPSILON)
        value = (wide * scale).astype(jnp.bfloat16)
        for s in range(n_fs):
            normed[s, at, :] = value[:, s * rows : (s + 1) * rows]
        acc[0, at, :] = jnp.zeros((tile, cols), jnp.float32)
        acc[1, at, :] = jnp.zeros((tile, cols), jnp.float32)
        return carry

    lax.fori_loop(0, 1, norm_tile, 0)
    send_own(*own[-1])
    lax.fori_loop(1, n_tokens // tile, norm_tile, 0)

    expert = tp * cols // FF
    top = logits.shape[0]
    score = [logits[k : k + 1, :] for k in range(top)]
    peak = functools.reduce(jnp.maximum, score)
    grown = [jnp.exp(x - peak) for x in score]
    whole = sum(grown)
    weight_col[...] = as_column(
        sum(jnp.where(routes[k : k + 1, :] == expert, grown[k] / whole, 0.0) for k in range(top))
    )

    wide_tile = min(512, cols)

    def project(a, s):
        block = pl.ds(pl.multiple_of(s * rows, rows), rows)

        def one(i, carry):
            at = pl.ds(pl.multiple_of(i * wide_tile, wide_tile), wide_tile)
            acc[a, :, at] += jnp.dot(
                normed[s], outs[a][block, at], preferred_element_type=jnp.float32
            )
            return carry

        lax.fori_loop(0, cols // wide_tile, one, 0)

    def wait_partner_line(a, s, r):
        copy(PARTNER, a, s, r).wait_recv()

    def wait_partner_block(a, s):
        for r in range(n_chunks):
            wait_partner_line(a, s, r)

    def project_pair(a, at_z):
        project(a, at_z * CORES + core)
        other = at_z * CORES + 1 - core
        wait_partner_block(a, other)
        project(a, other)

    def part_copy(s, r):
        first, size = table[2][r]
        start = s * rows + first
        owner, offset = start // per_owner, start % per_owner
        step = math.gcd(rows, first)
        return pltpu.make_async_remote_copy(
            src_ref=part.at[pl.ds(pl.multiple_of(start, step), size)],
            dst_ref=landed.at[tp, pl.ds(pl.multiple_of(offset, step), size)],
            send_sem=part_send.at[s, r],
            recv_sem=part_recv.at[tp, offset // rows, r],
            device_id={"tp": owner},
            device_id_type=MESH,
        )

    def down_rows(s, chunks):
        first, size = table[2][chunks[0]][0], sum(table[2][r][1] for r in chunks)
        start = s * rows + first
        step = math.gcd(rows, first)
        at = pl.ds(pl.multiple_of(start, step), size)
        value = lax.dot_general(
            outs[2][at, :], active[...], (((1,), (1,)), ((), ())),
            preferred_element_type=jnp.float32,
        ).astype(jnp.bfloat16)
        owner, offset = start // per_owner, start % per_owner

        @pl.when(owner == tp)
        def _():
            landed[tp, pl.ds(pl.multiple_of(offset, step), size), :] = value

        @pl.when(owner != tp)
        def _():
            part[at, :] = value
            for r in chunks:
                part_copy(s, r).start()

    def activate():
        def one(i, carry):
            at = pl.ds(pl.multiple_of(i * tile, tile), tile)
            active[at, :] = (
                weight_col[at, :] * clamped_unit(acc[0, at, :], acc[1, at, :])
            ).astype(jnp.bfloat16)
            return carry

        lax.fori_loop(0, n_tokens // tile, one, 0)

    def down_near(s, carry):
        at_z = s // CORES

        @pl.when(jnp.abs(at_z - z) < n_z - 1)
        def _():
            pl.when(s % CORES != core)(lambda: wait_partner_block(2, s))
            down_rows(s, range(n_chunks))

        return carry

    for a in range(2):
        project_pair(a, z)

    for d in range(1, n_z):
        last = d == n_z - 1
        for a in range(3):
            if last and a == 2:
                activate()
                lax.fori_loop(0, n_fs, down_near, 0)

            def arrive(r, a=a, d=d, last=last):
                for sign, inside, onward, more in (
                    (-1, z - d >= 0, RIGHT, z < n_z - 1),
                    (1, z + d < n_z, LEFT, z > 0),
                ):

                    @pl.when(inside)
                    def _():
                        at_z = z + sign * d
                        s = at_z * CORES + core
                        copy(onward, a, s, r).wait_recv()
                        pl.when(more)(lambda: copy(onward, a, s, r).start())
                        copy(PARTNER, a, s, r).start()
                        if last and a == 2:
                            other = at_z * CORES + 1 - core
                            down_rows(s, (r,))
                            wait_partner_line(a, other, r)
                            down_rows(other, (r,))

            for r in range(n_chunks):
                arrive(r)
            if a < 2:
                pl.when(z - d >= 0)(lambda a=a, d=d: project_pair(a, z - d))
                pl.when(z + d < n_z)(lambda a=a, d=d: project_pair(a, z + d))

    def sent(s, carry):
        at_z = s // CORES

        @pl.when(s % CORES == core)
        def _():
            for a in range(3):
                for r in range(n_chunks):
                    copy(PARTNER, a, s, r).wait_send()

            @pl.when((z > 0) & (at_z >= z))
            def _():
                for a in range(3):
                    for r in range(n_chunks):
                        copy(LEFT, a, s, r).wait_send()

            @pl.when((z < n_z - 1) & (at_z <= z))
            def _():
                for a in range(3):
                    for r in range(n_chunks):
                        copy(RIGHT, a, s, r).wait_send()

        @pl.when(s * rows // per_owner != tp)
        def _():
            for r in range(n_chunks):
                part_copy(s, r).wait_send()

        return carry

    lax.fori_loop(0, n_fs, sent, 0)

    group = min(128, rows)
    done = 0
    for r in range(n_chunks):
        first, size = table[2][r]
        for j in range(per_owner // rows):
            for step in range(1, n_tp):
                sender = lax.rem(tp + step, n_tp)
                spot = landed.at[sender, pl.ds(j * rows + first, size)]
                pltpu.make_async_remote_copy(
                    src_ref=spot, dst_ref=spot, send_sem=part_send.at[0, 0],
                    recv_sem=part_recv.at[sender, j, r],
                    device_id={"tp": sender}, device_id_type=MESH,
                ).wait_recv()
        while done + group <= first + size:
            for j in range(per_owner // rows):
                at = slice(j * rows + done, j * rows + done + group)
                total = landed[0, at, :].astype(jnp.float32)
                for p in range(1, n_tp):
                    total += landed[p, at, :].astype(jnp.float32)
                moe_out[:, at] = jnp.transpose(total).astype(jnp.bfloat16)
            done += group


def write_out(*refs):
    count = (len(refs) - 1) // 2
    sources, targets, sem = refs[:count], refs[count:-1], refs[-1]
    copies = [
        pltpu.make_async_copy(source, target, sem.at[i])
        for i, (source, target) in enumerate(zip(sources, targets))
    ]
    for copy in copies:
        copy.start()
    for copy in copies:
        copy.wait()


def on_device(n_fs, n_tp, tokens, routes, logits, gain, gate_w, up_w, down_w):
    rows, cols = gate_w.shape
    n_tokens, width = tokens.shape
    per_owner = width // n_tp
    n_chunks = len(cuts(rows)[0])
    full = pltpu.VMEM((rows * n_fs, cols), jnp.bfloat16)
    vmem = pl.BlockSpec(memory_space=pltpu.VMEM)
    hbm = pl.BlockSpec(memory_space=pl.ANY)
    held = pl.pallas_call(
        functools.partial(kernel, n_fs, n_tp),
        out_shape=(full, full, full, pltpu.VMEM((n_tokens, per_owner), jnp.bfloat16)),
        in_specs=[vmem] * 4 + [hbm] * 3,
        out_specs=(vmem,) * 4,
        scratch_shapes=[
            pltpu.VMEM((3, rows, cols), jnp.float32),
            pltpu.VMEM((rows, 1), jnp.float32),
            pltpu.VMEM((n_tokens, 1), jnp.float32),
            pltpu.VMEM((n_fs, n_tokens, rows), jnp.bfloat16),
            pltpu.VMEM((2, n_tokens, cols), jnp.float32),
            pltpu.VMEM((n_tokens, cols), jnp.bfloat16),
            pltpu.VMEM((width, n_tokens), jnp.bfloat16),
            pltpu.VMEM((n_tp, per_owner, n_tokens), jnp.bfloat16),
            pltpu.SemaphoreType.DMA((3, n_chunks)),
            pltpu.SemaphoreType.DMA((3, 3, n_fs // CORES, n_chunks)),
            pltpu.SemaphoreType.DMA((3, n_fs, n_chunks)),
            pltpu.SemaphoreType.DMA((n_fs, n_chunks)),
            pltpu.SemaphoreType.DMA((n_tp, per_owner // rows, n_chunks)),
        ],
        compiler_params=pltpu.CompilerParams(
            collective_id=0, has_side_effects=True, vmem_limit_bytes=34 * 2**20
        ),
    )(tokens, routes.T, logits.T, gain.reshape(1, rows), gate_w, up_w, down_w)
    return tuple(pl.pallas_call(
        write_out,
        out_shape=tuple(jax.ShapeDtypeStruct(x.shape, x.dtype) for x in held),
        in_specs=[hbm] * 4,
        out_specs=(hbm,) * 4,
        scratch_shapes=[pltpu.SemaphoreType.DMA((4,))],
        compiler_params=pltpu.CompilerParams(vmem_limit_bytes=2**20),
    )(*held))


def solution(mesh):
    return jax.shard_map(
        functools.partial(on_device, mesh.shape["fs"], mesh.shape["tp"]),
        mesh=mesh,
        in_specs=(
            P("fs", None),
            P("fs", None),
            P("fs", None),
            P("fs"),
            P("fs", "tp"),
            P("fs", "tp"),
            P("fs", "tp"),
        ),
        out_specs=(P(None, "tp"), P(None, "tp"), P(None, "tp"), P("fs", "tp")),
        check_vma=False,
    )
```

```python
import functools
import math

import jax
import jax.numpy as jnp
from jax import lax
from jax.experimental import pallas as pl
from jax.experimental.pallas import tpu as pltpu
from jax.sharding import PartitionSpec as P

FF = 2048
CORES = 2

EPSILON = 1e-06
CLAMP_LIMIT = 7.0
SIGMOID_SCALE = 1.702
MESH = pl.DeviceIdType.MESH
LEFT, RIGHT, PARTNER = range(3)


def clamped_unit(pre_gate, pre_up):
    gated = jnp.minimum(pre_gate, CLAMP_LIMIT)
    upper = jnp.clip(pre_up, -CLAMP_LIMIT, CLAMP_LIMIT)
    return gated * jax.nn.sigmoid(SIGMOID_SCALE * gated) * (upper + 1.0)


def as_column(row):
    n = row.shape[1]
    here = lax.broadcasted_iota(jnp.int32, (n, n), 0)
    there = lax.broadcasted_iota(jnp.int32, (n, n), 1)
    spread = jnp.where(here == there, jnp.broadcast_to(row, (n, n)), 0.0)
    return jnp.sum(spread, axis=1, keepdims=True)


def cuts(rows):
    if rows % 256:
        return [[(0, rows)]] * 3
    tables = []
    for parts in ((1, 2, 2, 3), (2, 2, 2, 2), (2, 2, 3, 1)):
        table, start = [], 0
        for part in parts:
            table.append((start, part * rows // 8))
            start += part * rows // 8
        tables.append(table)
    return tables


def kernel(
    n_fs, n_tp,
    tokens, routes, logits, gain, gate_w, up_w, down_w,
    gate_out, up_out, down_out, moe_out,
    staged, gain_col, weight_col, normed, acc, active, part, landed,
    load_sem, send_sem, recv_sem, part_send, part_recv,
):
    me, tp = lax.axis_index("fs"), lax.axis_index("tp")
    z, core = me // CORES, me % CORES
    n_z = n_fs // CORES
    partner = z * CORES + (1 - core)
    weights, outs = (gate_w, up_w, down_w), (gate_out, up_out, down_out)
    rows, cols = gate_w.shape
    n_tokens, width = tokens.shape
    table = cuts(rows)
    n_chunks = len(table[0])
    per_owner = width // n_tp

    barrier = pltpu.get_barrier_semaphore()

    def greet(device):
        pl.semaphore_signal(barrier, inc=1, device_id=device, device_id_type=MESH)

    pl.when(z > 0)(lambda: greet({"fs": me - CORES}))
    pl.when(z < n_z - 1)(lambda: greet({"fs": me + CORES}))
    greet({"fs": partner})
    for step in range(1, n_tp):
        greet({"tp": lax.rem(tp + step, n_tp)})

    def load(a, r):
        return pltpu.make_async_copy(
            weights[a].at[pl.ds(*table[a][r])],
            staged.at[a, pl.ds(*table[a][r])],
            load_sem.at[a, r],
        )

    for a in range(3):
        for r in range(n_chunks):
            load(a, r).start()

    gain_col[...] = as_column(gain[...])

    def place(a, s, r):
        first, size = table[a][r]
        return pl.ds(pl.multiple_of(s * rows + first, math.gcd(rows, first)), size)

    def copy(kind, a, s, r):
        target = (me - CORES, me + CORES, partner)[kind]
        return pltpu.make_async_remote_copy(
            src_ref=outs[a].at[place(a, s, r)],
            dst_ref=outs[a].at[place(a, s, r)],
            send_sem=send_sem.at[kind, a, s // CORES, r],
            recv_sem=recv_sem.at[a, s, r],
            device_id={"fs": target},
            device_id_type=MESH,
        )

    def send_own(a, r):
        pl.when(z > 0)(lambda: copy(LEFT, a, me, r).start())
        pl.when(z < n_z - 1)(lambda: copy(RIGHT, a, me, r).start())
        copy(PARTNER, a, me, r).start()

    own = [(a, r) for a in range(3) for r in range(n_chunks)]
    for i, (a, r) in enumerate(own):
        load(a, r).wait()
        at = pl.ds(*table[a][r])
        block = staged[a, at, :]
        if a < 2:
            block = gain_col[at, :] * block
        outs[a][place(a, me, r), :] = block.astype(jnp.bfloat16)
        if i == 0:
            pl.semaphore_wait(
                barrier,
                n_tp + (z > 0).astype(jnp.int32) + (z < n_z - 1).astype(jnp.int32),
            )
        else:
            send_own(*own[i - 1])

    tile = min(32, n_tokens)

    def norm_tile(i, carry):
        at = pl.ds(pl.multiple_of(i * tile, tile), tile)
        wide = tokens[at, :].astype(jnp.float32)
        scale = lax.rsqrt(jnp.mean(wide * wide, axis=-1, keepdims=True) + EPSILON)
        value = (wide * scale).astype(jnp.bfloat16)
        for s in range(n_fs):
            normed[s, at, :] = value[:, s * rows : (s + 1) * rows]
        acc[0, at, :] = jnp.zeros((tile, cols), jnp.float32)
        acc[1, at, :] = jnp.zeros((tile, cols), jnp.float32)
        return carry

    lax.fori_loop(0, 1, norm_tile, 0)
    send_own(*own[-1])
    lax.fori_loop(1, n_tokens // tile, norm_tile, 0)

    expert = tp * cols // FF
    top = logits.shape[0]
    score = [logits[k : k + 1, :] for k in range(top)]
    peak = functools.reduce(jnp.maximum, score)
    grown = [jnp.exp(x - peak) for x in score]
    whole = sum(grown)
    weight_col[...] = as_column(
        sum(jnp.where(routes[k : k + 1, :] == expert, grown[k] / whole, 0.0) for k in range(top))
    )

    wide_tile = min(512, cols)

    def project(a, s):
        block = pl.ds(pl.multiple_of(s * rows, rows), rows)

        def one(i, carry):
            at = pl.ds(pl.multiple_of(i * wide_tile, wide_tile), wide_tile)
            acc[a, :, at] += jnp.dot(
                normed[s], outs[a][block, at], preferred_element_type=jnp.float32
            )
            return carry

        lax.fori_loop(0, cols // wide_tile, one, 0)

    def wait_partner_line(a, s, r):
        copy(PARTNER, a, s, r).wait_recv()

    def wait_partner_block(a, s):
        for r in range(n_chunks):
            wait_partner_line(a, s, r)

    def project_pair(a, at_z):
        project(a, at_z * CORES + core)
        other = at_z * CORES + 1 - core
        wait_partner_block(a, other)
        project(a, other)

    def part_copy(s, r):
        first, size = table[2][r]
        start = s * rows + first
        owner, offset = start // per_owner, start % per_owner
        step = math.gcd(rows, first)
        return pltpu.make_async_remote_copy(
            src_ref=part.at[pl.ds(pl.multiple_of(start, step), size)],
            dst_ref=landed.at[tp, pl.ds(pl.multiple_of(offset, step), size)],
            send_sem=part_send.at[s, r],
            recv_sem=part_recv.at[tp, offset // rows, r],
            device_id={"tp": owner},
            device_id_type=MESH,
        )

    def down_rows(s, chunks):
        first, size = table[2][chunks[0]][0], sum(table[2][r][1] for r in chunks)
        start = s * rows + first
        step = math.gcd(rows, first)
        at = pl.ds(pl.multiple_of(start, step), size)
        value = jnp.dot(
            outs[2][at, :], active[...], preferred_element_type=jnp.float32
        ).astype(jnp.bfloat16)
        owner, offset = start // per_owner, start % per_owner

        @pl.when(owner == tp)
        def _():
            landed[tp, pl.ds(pl.multiple_of(offset, step), size), :] = value

        @pl.when(owner != tp)
        def _():
            part[at, :] = value
            for r in chunks:
                part_copy(s, r).start()

    def activate():
        token_tile = min(128, n_tokens)
        col_tiles = cols // wide_tile

        def one(i, carry):
            at = pl.ds(pl.multiple_of(i // col_tiles * token_tile, token_tile), token_tile)
            to = pl.ds(pl.multiple_of(i % col_tiles * wide_tile, wide_tile), wide_tile)
            value = weight_col[at, :] * clamped_unit(acc[0, at, to], acc[1, at, to])
            active[to, at] = jnp.transpose(value).astype(jnp.bfloat16)
            return carry

        lax.fori_loop(0, n_tokens // token_tile * col_tiles, one, 0)

    def down_near(s, carry):
        at_z = s // CORES

        @pl.when(jnp.abs(at_z - z) < n_z - 1)
        def _():
            pl.when(s % CORES != core)(lambda: wait_partner_block(2, s))
            down_rows(s, range(n_chunks))

        return carry

    for a in range(2):
        project_pair(a, z)

    for d in range(1, n_z):
        last = d == n_z - 1
        for a in range(3):
            if last and a == 2:
                activate()
                lax.fori_loop(0, n_fs, down_near, 0)

            def arrive(r, a=a, d=d, last=last):
                for sign, inside, onward, more in (
                    (-1, z - d >= 0, RIGHT, z < n_z - 1),
                    (1, z + d < n_z, LEFT, z > 0),
                ):

                    @pl.when(inside)
                    def _():
                        at_z = z + sign * d
                        s = at_z * CORES + core
                        copy(onward, a, s, r).wait_recv()
                        pl.when(more)(lambda: copy(onward, a, s, r).start())
                        copy(PARTNER, a, s, r).start()
                        if last and a == 2:
                            other = at_z * CORES + 1 - core
                            down_rows(s, (r,))
                            wait_partner_line(a, other, r)
                            down_rows(other, (r,))

            for r in range(n_chunks):
                arrive(r)
            if a < 2:
                pl.when(z - d >= 0)(lambda a=a, d=d: project_pair(a, z - d))
                pl.when(z + d < n_z)(lambda a=a, d=d: project_pair(a, z + d))

    def sent(s, carry):
        at_z = s // CORES

        @pl.when(s % CORES == core)
        def _():
            for a in range(3):
                for r in range(n_chunks):
                    copy(PARTNER, a, s, r).wait_send()

            @pl.when((z > 0) & (at_z >= z))
            def _():
                for a in range(3):
                    for r in range(n_chunks):
                        copy(LEFT, a, s, r).wait_send()

            @pl.when((z < n_z - 1) & (at_z <= z))
            def _():
                for a in range(3):
                    for r in range(n_chunks):
                        copy(RIGHT, a, s, r).wait_send()

        @pl.when(s * rows // per_owner != tp)
        def _():
            for r in range(n_chunks):
                part_copy(s, r).wait_send()

        return carry

    lax.fori_loop(0, n_fs, sent, 0)

    group = min(128, rows)
    done = 0
    for r in range(n_chunks):
        first, size = table[2][r]
        for j in range(per_owner // rows):
            for step in range(1, n_tp):
                sender = lax.rem(tp + step, n_tp)
                spot = landed.at[sender, pl.ds(j * rows + first, size)]
                pltpu.make_async_remote_copy(
                    src_ref=spot, dst_ref=spot, send_sem=part_send.at[0, 0],
                    recv_sem=part_recv.at[sender, j, r],
                    device_id={"tp": sender}, device_id_type=MESH,
                ).wait_recv()
        while done + group <= first + size:
            for j in range(per_owner // rows):
                at = slice(j * rows + done, j * rows + done + group)
                total = landed[0, at, :].astype(jnp.float32)
                for p in range(1, n_tp):
                    total += landed[p, at, :].astype(jnp.float32)
                moe_out[:, at] = jnp.transpose(total).astype(jnp.bfloat16)
            done += group


def write_out(*refs):
    count = (len(refs) - 1) // 2
    sources, targets, sem = refs[:count], refs[count:-1], refs[-1]
    copies = [
        pltpu.make_async_copy(source, target, sem.at[i])
        for i, (source, target) in enumerate(zip(sources, targets))
    ]
    for copy in copies:
        copy.start()
    for copy in copies:
        copy.wait()


def on_device(n_fs, n_tp, tokens, routes, logits, gain, gate_w, up_w, down_w):
    rows, cols = gate_w.shape
    n_tokens, width = tokens.shape
    per_owner = width // n_tp
    n_chunks = len(cuts(rows)[0])
    full = pltpu.VMEM((rows * n_fs, cols), jnp.bfloat16)
    vmem = pl.BlockSpec(memory_space=pltpu.VMEM)
    hbm = pl.BlockSpec(memory_space=pl.ANY)
    held = pl.pallas_call(
        functools.partial(kernel, n_fs, n_tp),
        out_shape=(full, full, full, pltpu.VMEM((n_tokens, per_owner), jnp.bfloat16)),
        in_specs=[vmem] * 4 + [hbm] * 3,
        out_specs=(vmem,) * 4,
        scratch_shapes=[
            pltpu.VMEM((3, rows, cols), jnp.float32),
            pltpu.VMEM((rows, 1), jnp.float32),
            pltpu.VMEM((n_tokens, 1), jnp.float32),
            pltpu.VMEM((n_fs, n_tokens, rows), jnp.bfloat16),
            pltpu.VMEM((2, n_tokens, cols), jnp.float32),
            pltpu.VMEM((cols, n_tokens), jnp.bfloat16),
            pltpu.VMEM((width, n_tokens), jnp.bfloat16),
            pltpu.VMEM((n_tp, per_owner, n_tokens), jnp.bfloat16),
            pltpu.SemaphoreType.DMA((3, n_chunks)),
            pltpu.SemaphoreType.DMA((3, 3, n_fs // CORES, n_chunks)),
            pltpu.SemaphoreType.DMA((3, n_fs, n_chunks)),
            pltpu.SemaphoreType.DMA((n_fs, n_chunks)),
            pltpu.SemaphoreType.DMA((n_tp, per_owner // rows, n_chunks)),
        ],
        compiler_params=pltpu.CompilerParams(
            collective_id=0, has_side_effects=True, vmem_limit_bytes=34 * 2**20
        ),
    )(tokens, routes.T, logits.T, gain.reshape(1, rows), gate_w, up_w, down_w)
    return tuple(pl.pallas_call(
        write_out,
        out_shape=tuple(jax.ShapeDtypeStruct(x.shape, x.dtype) for x in held),
        in_specs=[hbm] * 4,
        out_specs=(hbm,) * 4,
        scratch_shapes=[pltpu.SemaphoreType.DMA((4,))],
        compiler_params=pltpu.CompilerParams(vmem_limit_bytes=2**20),
    )(*held))


def solution(mesh):
    return jax.shard_map(
        functools.partial(on_device, mesh.shape["fs"], mesh.shape["tp"]),
        mesh=mesh,
        in_specs=(
            P("fs", None),
            P("fs", None),
            P("fs", None),
            P("fs"),
            P("fs", "tp"),
            P("fs", "tp"),
            P("fs", "tp"),
        ),
        out_specs=(P(None, "tp"), P(None, "tp"), P(None, "tp"), P("fs", "tp")),
        check_vma=False,
    )
```
